32 devices in a mesh: kv: 8 (over z, x), tp: 4 (over y, core).
Axes of the slice: x: 2, y: 2, z: 4, core: 2. Of those that a mesh axis runs over, the one named last changes fastest.
Arguments:
- tokens: bfloat16 [64, 2048], P(None, 'kv'), may hold values from -16 to 16
- norm_gain: float32 [2048], P('kv'), may hold values from 0.1 to 1.9
- query_weight: bfloat16 [2048, 2048], P('kv', 'tp'), may hold values from -0.125 to 0.125
- key_weight: bfloat16 [2048, 2048], P('kv', 'tp'), may hold values from -0.125 to 0.125
- value_weight: bfloat16 [2048, 2048], P('kv', 'tp'), may hold values from -0.125 to 0.125
- gate_weight: bfloat16 [2048, 2048], P('kv', 'tp'), may hold values from -0.125 to 0.125
- beta_weight: bfloat16 [2048, 16], replicated, may hold values from -0.125 to 0.125
- decay_weight: bfloat16 [2048, 16], replicated, may hold values from -0.5 to 0.5
- decay_rate: float32 [16], P('tp'), may hold values from 0.0005 to 0.1
- head_gain: float32 [128], replicated, may hold values from 0.1 to 1.9
- carried_state: float32 [64, 16, 128, 128], P('kv', 'tp'), may hold values from -4 to 4
- block_keys: bfloat16 [64, 16, 64, 128], P('kv', 'tp'), may hold values from -1 to 1, as said below
- block_values: bfloat16 [64, 16, 64, 128], P('kv', 'tp'), may hold values from -6 to 6
- block_beta: float32 [64, 16, 64], P('kv', 'tp'), may hold values from 0.1 to 0.9
- block_decay: float32 [64, 16, 64], P('kv', 'tp'), may hold values from -1.2 to 0
- live_count: int32 [64], P('kv'), may hold values from 1 to 64, 1638 in all
- out_weight: bfloat16 [2048, 2048], P('tp', 'kv'), may hold values from -0.125 to 0.125
- mlp_gain: float32 [2048], replicated, may hold values from 0.1 to 1.9
- up_weight: bfloat16 [2048, 8192], P('kv', 'tp'), may hold values from -0.125 to 0.125
- down_weight: bfloat16 [8192, 2048], P('tp', 'kv'), may hold values from -0.0625 to 0.0625
Outputs:
- mixed: bfloat16 [64, 2048], P(None, 'kv')
- new_state: float32 [64, 16, 128, 128], P('kv', 'tp')
The draws below stay inside these ranges and needn't reach their ends.
Inputs may be any that keep to these rules, and one draw needn't show every extreme that they name: `block_keys`: every key vector along the last dimension has unit length up to rounding.
All inputs are finite; a program needn't handle non-finite values. No bound on the sum of `live_count` on one device may be relied on, other than what follows from the above.
Results may differ from the reference program's by a relative error of at most 0.023.
Values may be sent and summed in bfloat16 or wider, within the bound.
A program may use at most 64 MiB of HBM per device.

```python
import math
import jax
import jax.numpy as jnp
import numpy as np
from jax import lax

MODEL = 2048
HEADS = 16
HEAD_DIM = 128
MLP_UNITS = 8192
BLOCK_POSITIONS = 64
SEQ_DEV = 8
BATCH_TOTAL = 64
N_KV = 8
N_TP = 4


def head_rates(key):
    key_pick, key_fast, key_slow = jax.random.split(jax.random.fold_in(key, 11), 3)
    fast_heads = jax.random.randint(key_pick, (HEADS,), 0, 2) == 1
    fast_rate = jnp.exp(jax.random.uniform(key_fast, (HEADS,), jnp.float32, jnp.log(0.03), jnp.log(0.1)))
    slow_rate = jnp.exp(jax.random.uniform(key_slow, (HEADS,), jnp.float32, jnp.log(0.001), jnp.log(0.01)))
    return jnp.where(fast_heads, fast_rate, slow_rate)


def draw_decay_rate(key, part):
    return head_rates(key).astype(jnp.float32)


def draw_block_decay(key, part):
    decay_rates = head_rates(key)
    sequence_multiplier = jnp.exp(jax.random.uniform(jax.random.fold_in(key, 12), (BATCH_TOTAL, 1, 1), jnp.float32, jnp.log(0.5), jnp.log(2.0)))
    coarse_multiplier = jnp.exp(jax.random.uniform(jax.random.fold_in(key, 13), (BATCH_TOTAL, HEADS, BLOCK_POSITIONS), jnp.float32, jnp.log(0.3), jnp.log(2.0)))
    spike_selector = jax.random.randint(jax.random.fold_in(key, 14), (BATCH_TOTAL, 1, BLOCK_POSITIONS), 0, BLOCK_POSITIONS // 2) == 0
    spike_penalty = jnp.log(jax.random.uniform(jax.random.fold_in(key, 15), (BATCH_TOTAL, 1, BLOCK_POSITIONS), jnp.float32, 0.5, 0.8))
    decay_logarithm = -(decay_rates[None, :, None] * sequence_multiplier * coarse_multiplier) + jnp.where(spike_selector, spike_penalty, 0.0)
    return decay_logarithm.astype(jnp.float32)


def draw_block_keys(key, part):
    key_shared, key_noise = jax.random.split(jax.random.fold_in(key, 21))
    shared_shape = (BATCH_TOTAL, HEADS, 1, HEAD_DIM)
    noise_shape = (BATCH_TOTAL, HEADS, BLOCK_POSITIONS, HEAD_DIM)
    shared = jax.random.normal(key_shared, shared_shape, jnp.float32)
    noise = jax.random.normal(key_noise, noise_shape, jnp.float32)
    raw_keys = 0.6 * shared + 0.8 * noise
    lengths_sq = jnp.sum(raw_keys * raw_keys, axis=3, keepdims=True) + 1e-06
    return (raw_keys / jnp.sqrt(lengths_sq)).astype(jnp.bfloat16)


def draw_tokens(key, part):
    key_rough, key_vals = jax.random.split(key, 2)
    column_ramp = jnp.exp(jnp.log(4.0) * jnp.arange(MODEL, dtype=jnp.float32) / MODEL)
    rough_scale = jnp.exp(jax.random.uniform(key_rough, (MODEL,), jnp.float32, -0.5, 0.5))
    entries = jax.random.normal(key_vals, (BATCH_TOTAL, MODEL), jnp.float32)
    return jnp.clip(entries * column_ramp * rough_scale * 0.6, -16.0, 16.0).astype(jnp.bfloat16)


def block_scale(key, shape, shards, low, top_value):
    level, own = 1.0, jax.random.fold_in(key, 6)
    for dim, shards_of in shards:
        steps = jnp.exp(jax.random.uniform(jax.random.fold_in(own, dim), (shards_of,), jnp.float32, low / len(shards), top_value / len(shards)))
        level = level * jnp.repeat(steps, shape[dim] // shards_of).reshape([-1 if axis == dim else 1 for axis in range(len(shape))])
    return level


def split_up(count, total, reach, lean):
    portions = [(1 << 20) // math.isqrt(grade ** lean) + 1 for grade in range(2, count + 1)]
    rest, counts = total - reach - (count - 1), [1] * (count - 1)
    while rest > 0:
        free = [i for i in range(count - 1) if counts[i] < reach]
        whole, budget = sum([portions[i] for i in free]), rest
        for i in free:
            extra = min(reach - counts[i], max(1, budget * portions[i] // whole), rest)
            counts[i] = counts[i] + extra
            rest = rest - extra
    return np.array([reach] + counts)


def ragged(key, amount, total, most, lean):
    if amount == 2:
        one = jax.random.randint(key, (), max(1, total - most), min(most, total - 1) + 1)
        return jnp.stack([one, total - one])
    sizes = jnp.asarray(split_up(amount, total, most, lean), jnp.int32)
    couples = (amount - 1) // 2
    giver, receiver = sizes[1:1 + 2 * couples:2], sizes[2:2 + 2 * couples:2]
    margin = jnp.minimum(giver - 1, most - receiver)
    moved = jax.random.randint(jax.random.fold_in(key, 1), (couples,), 0, 1 << 20) % (margin + 1)
    sizes = sizes.at[1:1 + 2 * couples:2].set(giver - moved).at[2:2 + 2 * couples:2].set(receiver + moved)
    return sizes[jax.random.permutation(jax.random.fold_in(key, 2), amount)]


def scatter_about(own_key, shape, deviation, bound, pieces=(), held_as=jnp.bfloat16):
    drawn = deviation * jax.random.normal(own_key, shape, jnp.float32)
    if pieces:
        drawn = drawn * block_scale(own_key, shape, pieces, -0.22, 0.18)
    return jnp.clip(drawn, -bound, bound).astype(held_as)


def setup_inputs(seed: int = 0) -> dict:
    key_of = jax.random.split(jax.random.key(seed), 21)
    return {
        "tokens": draw_tokens(jax.random.fold_in(key_of[20], 71), 0),
        "norm_gain": jnp.clip(1.0 + 0.18 * jax.random.normal(key_of[1], (MODEL,), jnp.float32), 0.1, 1.9),
        "query_weight": scatter_about(key_of[2], (MODEL, HEADS * HEAD_DIM), MODEL ** -0.5, 0.125, ((0, 8), (1, 4))),
        "key_weight": scatter_about(key_of[3], (MODEL, HEADS * HEAD_DIM), MODEL ** -0.5, 0.125, ((0, 8), (1, 4))),
        "value_weight": scatter_about(key_of[4], (MODEL, HEADS * HEAD_DIM), MODEL ** -0.5, 0.125, ((0, 8), (1, 4))),
        "gate_weight": scatter_about(key_of[5], (MODEL, HEADS * HEAD_DIM), MODEL ** -0.5, 0.125, ((0, 8), (1, 4))),
        "beta_weight": scatter_about(key_of[6], (MODEL, HEADS), MODEL ** -0.5, 0.125),
        "decay_weight": scatter_about(key_of[7], (MODEL, HEADS), (MODEL // 16) ** -0.5, 0.5),
        "decay_rate": draw_decay_rate(jax.random.fold_in(key_of[20], 71), 0),
        "head_gain": jnp.clip(1.0 + 0.18 * jax.random.normal(key_of[9], (HEAD_DIM,), jnp.float32), 0.1, 1.9),
        "carried_state": scatter_about(key_of[10], (BATCH_TOTAL, HEADS, HEAD_DIM, HEAD_DIM), 0.3, 4.0, ((0, 8), (1, 4)), jnp.float32),
        "block_keys": draw_block_keys(jax.random.fold_in(key_of[20], 71), 0),
        "block_values": scatter_about(key_of[12], (BATCH_TOTAL, HEADS, BLOCK_POSITIONS, HEAD_DIM), 1.0, 6.0, ((0, 8), (1, 4))),
        "block_beta": jnp.clip(0.1 + 0.79999997 * jax.random.uniform(key_of[13], (BATCH_TOTAL, HEADS, BLOCK_POSITIONS), jnp.float32) ** block_scale(key_of[13], (BATCH_TOTAL, HEADS, BLOCK_POSITIONS), ((0, 8), (1, 4)), -0.2, 0.2), 0.1, 0.9),
        "block_decay": draw_block_decay(jax.random.fold_in(key_of[20], 71), 0),
        "live_count": ragged(key_of[15], BATCH_TOTAL, BATCH_TOTAL * BLOCK_POSITIONS * 2 // 5, BLOCK_POSITIONS, 2).astype(jnp.int32),
        "out_weight": scatter_about(key_of[16], (HEADS * HEAD_DIM, MODEL), (HEADS * HEAD_DIM) ** -0.5, 0.125, ((0, 4), (1, 8))),
        "mlp_gain": jnp.clip(1.0 + 0.18 * jax.random.normal(key_of[17], (MODEL,), jnp.float32), 0.1, 1.9),
        "up_weight": scatter_about(key_of[18], (MODEL, MLP_UNITS), MODEL ** -0.5, 0.125, ((0, 8), (1, 4))),
        "down_weight": scatter_about(key_of[19], (MLP_UNITS, MODEL), MLP_UNITS ** -0.5, 0.0625, ((0, 4), (1, 8))),
    }


EPS = 1e-06
PRECISE = lax.Precision.HIGHEST

def unit_inverse(strict_lower):
    slots_count = strict_lower.shape[-1]
    identity = jnp.eye(slots_count, dtype=strict_lower.dtype)
    powered = -strict_lower
    product_sum = identity + powered
    for repeat in range(slots_count.bit_length() - 2):
        powered = jnp.matmul(powered, powered, precision=PRECISE)
        product_sum = product_sum + jnp.matmul(product_sum, powered, precision=PRECISE)
    return product_sum

def delta_block(queries, key_new, value_new, beta_new, decay_new, keys, values, betas, decays, live_count, carried_state):
    slots_count = keys.shape[2]
    slot_ids = jnp.arange(slots_count, dtype=jnp.int32)
    newest = (live_count.astype(jnp.int32) - 1)[:, None, None]
    pending = slot_ids[None, None, :] < newest
    current = slot_ids[None, None, :] == newest
    keys_all = jnp.where(pending[..., None], keys, jnp.where(current[..., None], key_new[:, :, None, :], jnp.zeros_like(keys)))
    values_all = jnp.where(pending[..., None], values, jnp.where(current[..., None], value_new[:, :, None, :], jnp.zeros_like(values)))
    betas_all = jnp.where(pending, betas, jnp.where(current, beta_new[:, :, None], 0.0))
    decays_all = jnp.where(pending, decays, jnp.where(current, decay_new[:, :, None], 0.0))
    totals = jnp.cumsum(decays_all, axis=2)
    strict = slot_ids[:, None] > slot_ids[None, :]
    spread = jnp.where(strict, totals[..., :, None] - totals[..., None, :], 0.0)
    key_vals = keys_all.astype(jnp.float32)
    intersection = jnp.einsum('shid,shjd->shij', key_vals, key_vals, precision=PRECISE)
    strict_lower = jnp.where(strict, betas_all[..., :, None] * intersection * jnp.exp(spread), 0.0)
    inverse = unit_inverse(strict_lower)
    right_values = betas_all[..., None] * values_all.astype(jnp.float32)
    right_keys = (betas_all * jnp.exp(totals))[..., None] * key_vals
    solved_values = jnp.einsum('shij,shjv->shiv', inverse, right_values, precision=PRECISE)
    solved_keys = jnp.einsum('shij,shjk->shik', inverse, right_keys, precision=PRECISE)
    update = solved_values - jnp.einsum('shik,shkv->shiv', solved_keys, carried_state, precision=PRECISE)
    ending = totals[..., -1]
    faded_keys = key_vals * jnp.exp(ending[..., None] - totals)[..., None]
    new_state = jnp.exp(ending)[..., None, None] * carried_state + jnp.einsum('shik,shiv->shkv', faded_keys, update, precision=PRECISE)
    readout = jnp.einsum('shk,shkv->shv', queries, new_state, precision=PRECISE)
    return (readout, new_state)

def reference(tokens, norm_gain, query_weight, key_weight, value_weight, gate_weight, beta_weight, decay_weight, decay_rate, head_gain, carried_state, block_keys, block_values, block_beta, block_decay, live_count, out_weight, mlp_gain, up_weight, down_weight):
    token_vals = tokens.astype(jnp.float32)
    inverse_rms = lax.rsqrt(lax.optimization_barrier(jnp.mean(token_vals * token_vals, axis=1)) + EPS)[:, None]
    normed = (token_vals * norm_gain).astype(jnp.bfloat16)

    def project(weight):
        return jnp.dot(normed, weight, preferred_element_type=jnp.float32) * inverse_rms
    queries = project(query_weight).reshape(BATCH_TOTAL, HEADS, HEAD_DIM)
    key_raw = project(key_weight).reshape(BATCH_TOTAL, HEADS, HEAD_DIM)
    value_raw = project(value_weight).reshape(BATCH_TOTAL, HEADS, HEAD_DIM)
    gate_raw = project(gate_weight).reshape(BATCH_TOTAL, HEADS, HEAD_DIM)
    beta_new = jax.nn.sigmoid(project(beta_weight))
    decay_new = -decay_rate * jax.nn.softplus(project(decay_weight))
    key_new = (key_raw * lax.rsqrt(lax.optimization_barrier(jnp.sum(key_raw * key_raw, axis=2, keepdims=True)) + EPS)).astype(jnp.bfloat16)
    value_new = value_raw.astype(jnp.bfloat16)

    def grouped(array):
        return array.reshape((N_KV, SEQ_DEV) + array.shape[1:])
    grouped_args = tuple((grouped(item) for item in (queries, key_new, value_new, beta_new, decay_new, block_keys, block_values, block_beta, block_decay, live_count, carried_state)))
    readout, new_state = lax.map(lambda member: delta_block(*member), grouped_args)
    readout = readout.reshape(BATCH_TOTAL, HEADS, HEAD_DIM)
    new_state = new_state.reshape(BATCH_TOTAL, HEADS, HEAD_DIM, HEAD_DIM)
    scaled = readout * lax.rsqrt(lax.optimization_barrier(jnp.mean(readout * readout, axis=2, keepdims=True)) + EPS) * head_gain
    mixed_heads = (scaled * jax.nn.silu(gate_raw)).reshape(BATCH_TOTAL, HEADS * HEAD_DIM).astype(jnp.bfloat16)
    heads_dev = HEADS // N_TP
    blocks_in = mixed_heads.reshape(BATCH_TOTAL, N_TP, heads_dev * HEAD_DIM).astype(jnp.float32)
    blocks_weight = out_weight.reshape(N_TP, heads_dev * HEAD_DIM, MODEL).astype(jnp.float32)
    partial_value = jnp.einsum('btj,tjd->tbd', blocks_in, blocks_weight, precision=PRECISE)
    partial_value = lax.optimization_barrier(partial_value.astype(jnp.bfloat16)).astype(jnp.float32)
    attended = lax.optimization_barrier(jnp.sum(partial_value, axis=0))
    residual = lax.optimization_barrier((token_vals + attended).astype(jnp.bfloat16))
    resid_vals = residual.astype(jnp.float32)
    mlp_rms = lax.rsqrt(lax.optimization_barrier(jnp.mean(resid_vals * resid_vals, axis=1)) + EPS)[:, None]
    mlp_in = (resid_vals * mlp_gain).astype(jnp.bfloat16)
    pre_act = jnp.dot(mlp_in, up_weight, preferred_element_type=jnp.float32) * mlp_rms
    hidden = jnp.square(jax.nn.relu(pre_act)).astype(jnp.bfloat16)
    mixed = (resid_vals + jnp.dot(hidden, down_weight, preferred_element_type=jnp.float32)).astype(jnp.bfloat16)
    return (mixed, new_state)
```

```python
import functools

import jax
import jax.numpy as jnp
from jax import lax
from jax.experimental import pallas as pl
from jax.experimental.pallas import tpu as pltpu
from jax.sharding import PartitionSpec as P

EPS = 1e-06
PRECISE = lax.Precision.HIGHEST


def unit_inverse(strict_lower):
    slots_count = strict_lower.shape[-1]
    identity = jnp.eye(slots_count, dtype=strict_lower.dtype)
    powered = -strict_lower
    product_sum = identity + powered
    for repeat in range(slots_count.bit_length() - 2):
        powered = jnp.matmul(powered, powered, precision=PRECISE)
        product_sum = product_sum + jnp.matmul(product_sum, powered, precision=PRECISE)
    return product_sum


def delta_block(
    queries,
    key_new,
    value_new,
    beta_new,
    decay_new,
    keys,
    values,
    betas,
    decays,
    live_count,
    carried_state,
):
    slots_count = keys.shape[2]
    slot_ids = jnp.arange(slots_count, dtype=jnp.int32)
    newest = (live_count - 1)[:, None, None]
    pending = slot_ids[None, None, :] < newest
    current = slot_ids[None, None, :] == newest
    keys_all = jnp.where(
        pending[..., None],
        keys,
        jnp.where(current[..., None], key_new[:, :, None, :], jnp.zeros_like(keys)),
    )
    values_all = jnp.where(
        pending[..., None],
        values,
        jnp.where(current[..., None], value_new[:, :, None, :], jnp.zeros_like(values)),
    )
    betas_all = jnp.where(pending, betas, jnp.where(current, beta_new[:, :, None], 0.0))
    decays_all = jnp.where(pending, decays, jnp.where(current, decay_new[:, :, None], 0.0))
    totals = jnp.cumsum(decays_all, axis=2)
    strict = slot_ids[:, None] > slot_ids[None, :]
    spread = jnp.where(strict, totals[..., :, None] - totals[..., None, :], 0.0)
    intersection = jnp.einsum(
        "shid,shjd->shij", keys_all, keys_all, preferred_element_type=jnp.float32
    )
    strict_lower = jnp.where(strict, betas_all[..., :, None] * intersection * jnp.exp(spread), 0.0)
    inverse = unit_inverse(strict_lower)
    key_vals = keys_all.astype(jnp.float32)
    right_values = betas_all[..., None] * values_all.astype(jnp.float32)
    right_keys = (betas_all * jnp.exp(totals))[..., None] * key_vals
    solved_values = jnp.einsum("shij,shjv->shiv", inverse, right_values, precision=PRECISE)
    solved_keys = jnp.einsum("shij,shjk->shik", inverse, right_keys, precision=PRECISE)
    update = solved_values - jnp.einsum(
        "shik,shkv->shiv", solved_keys, carried_state, precision=PRECISE
    )
    ending = totals[..., -1]
    faded_keys = key_vals * jnp.exp(ending[..., None] - totals)[..., None]
    new_state = jnp.exp(ending)[..., None, None] * carried_state + jnp.einsum(
        "shik,shiv->shkv", faded_keys, update, precision=PRECISE
    )
    readout = jnp.einsum("shk,shkv->shv", queries, new_state, precision=PRECISE)
    return (readout, new_state)


LANES = 128
MESH = pl.DeviceIdType.MESH
VMEM_SPEC = pl.BlockSpec(memory_space=pltpu.VMEM)
ANY_SPEC = pl.BlockSpec(memory_space=pl.ANY)


def greet(kv_size, tp_size):
    kv_index = lax.axis_index("kv")
    tp_index = lax.axis_index("tp")
    barrier = pltpu.get_barrier_semaphore()
    for step in range(1, kv_size):
        peer = lax.rem(kv_index + step, kv_size)
        pl.semaphore_signal(barrier, inc=1, device_id=(peer, tp_index), device_id_type=MESH)
    for step in range(1, tp_size):
        peer = lax.rem(tp_index + step, tp_size)
        pl.semaphore_signal(barrier, inc=1, device_id=(kv_index, peer), device_id_type=MESH)
    pl.semaphore_wait(barrier, kv_size - 1 + tp_size - 1)


def far_first(size):
    return sorted(range(1, size), key=lambda step: -min(step, size - step))


def send_all(axis, size, source_of, target, sends, receives):
    kv_index = lax.axis_index("kv")
    tp_index = lax.axis_index("tp")
    me = kv_index if axis == "kv" else tp_index
    copies = []
    for step in far_first(size):
        peer = lax.rem(me + step, size)
        copy = pltpu.make_async_remote_copy(
            src_ref=source_of(peer),
            dst_ref=target.at[me],
            send_sem=sends.at[step],
            recv_sem=receives.at[step],
            device_id=(peer, tp_index) if axis == "kv" else (kv_index, peer),
            device_id_type=MESH,
        )
        copy.start()
        copies.append(copy)
    return copies


def front_kernel(
    kv_size,
    model,
    tokens,
    norm_gain,
    query_weight,
    key_weight,
    value_weight,
    gate_weight,
    beta_weight,
    decay_weight,
    decay_rate,
    queries_out,
    key_out,
    value_out,
    gate_out,
    beta_out,
    decay_out,
    beta_rows,
    decay_rows,
    small,
    outgoing,
    incoming,
    local_sems,
    sends,
    receives,
):
    kv_index = lax.axis_index("kv")
    tp_index = lax.axis_index("tp")
    batch, columns = tokens.shape
    width = query_weight.shape[1]
    heads = beta_weight.shape[1]
    heads_here = decay_rate.shape[1]
    head_width = width // heads_here
    rows = batch // kv_size
    mine = pl.ds(kv_index * columns, columns)
    beta_copy = pltpu.make_async_copy(beta_weight.at[mine, :], beta_rows, local_sems.at[0])
    decay_copy = pltpu.make_async_copy(decay_weight.at[mine, :], decay_rows, local_sems.at[1])
    beta_copy.start()
    decay_copy.start()
    token_vals = tokens[...].astype(jnp.float32)
    squares = jnp.sum(token_vals * token_vals, axis=1, keepdims=True)
    normed = (token_vals * norm_gain[...]).astype(jnp.bfloat16)
    for place, weight in enumerate((query_weight, key_weight, value_weight, gate_weight)):
        product = jnp.dot(normed, weight[...], preferred_element_type=jnp.float32)
        outgoing[:, :, place * width : (place + 1) * width] = product.reshape(
            kv_size, rows, width
        ).astype(jnp.bfloat16)
    beta_copy.wait()
    decay_copy.wait()
    small[...] = jnp.zeros_like(small)
    small[:, 0:heads] = beta_rows[...]
    small[:, heads : 2 * heads] = decay_rows[...]
    gating = jnp.dot(normed, small[...], preferred_element_type=jnp.float32)
    lane = lax.broadcasted_iota(jnp.int32, gating.shape, 1)
    gating = jnp.where(lane == 2 * heads, squares, gating)
    outgoing[:, :, 4 * width :] = gating.reshape(kv_size, rows, LANES).astype(jnp.bfloat16)
    greet(kv_size, 1)
    copies = send_all("kv", kv_size, lambda peer: outgoing.at[peer], incoming, sends, receives)
    incoming[kv_index] = outgoing[kv_index]
    for copy in copies:
        copy.wait()

    def total(start, size):
        parts = incoming[:, :, start : start + size].astype(jnp.float32)
        return jnp.sum(parts, axis=0)

    gating = total(4 * width, LANES)
    inverse_rms = lax.rsqrt(gating[:, 2 * heads : 2 * heads + 1] / model + EPS)
    queries_out[...] = total(0, width) * inverse_rms
    key_raw = total(width, width) * inverse_rms
    for head in range(heads_here):
        span = slice(head * head_width, (head + 1) * head_width)
        one = key_raw[:, span]
        key_out[:, span] = (
            one * lax.rsqrt(jnp.sum(one * one, axis=1, keepdims=True) + EPS)
        ).astype(jnp.bfloat16)
    value_out[...] = (total(2 * width, width) * inverse_rms).astype(jnp.bfloat16)
    gate_raw = total(3 * width, width) * inverse_rms
    gate_out[...] = gate_raw * jax.nn.sigmoid(gate_raw)
    turn = lax.rem(LANES - tp_index * heads_here, LANES)
    gating = pltpu.roll(gating, turn, 1) * inverse_rms
    beta_out[...] = jax.nn.sigmoid(gating[:, 0:heads_here])
    raw = gating[:, heads : heads + heads_here]
    decay_out[...] = -decay_rate[...] * (
        jnp.maximum(raw, 0.0) + jnp.log1p(jnp.exp(-jnp.abs(raw)))
    )


def front(kv_size, tokens, norm_gain, projections, beta_weight, decay_weight, decay_rate):
    batch, columns = tokens.shape
    width = projections[0].shape[1]
    heads = beta_weight.shape[1]
    heads_here = decay_rate.shape[0]
    rows = batch // kv_size
    total = 4 * width + LANES
    float_out = jax.ShapeDtypeStruct((rows, width), jnp.float32)
    half_out = jax.ShapeDtypeStruct((rows, width), jnp.bfloat16)
    gate_shape = jax.ShapeDtypeStruct((rows, heads_here), jnp.float32)
    return pl.pallas_call(
        lambda *refs: front_kernel(kv_size, columns * kv_size, *refs),
        out_shape=(float_out, half_out, half_out, float_out, gate_shape, gate_shape),
        in_specs=[VMEM_SPEC] * 6 + [ANY_SPEC] * 2 + [VMEM_SPEC],
        out_specs=[VMEM_SPEC] * 6,
        scratch_shapes=[
            pltpu.VMEM((columns, heads), jnp.bfloat16),
            pltpu.VMEM((columns, heads), jnp.bfloat16),
            pltpu.VMEM((columns, LANES), jnp.bfloat16),
            pltpu.VMEM((kv_size, rows, total), jnp.bfloat16),
            pltpu.VMEM((kv_size, rows, total), jnp.bfloat16),
            pltpu.SemaphoreType.DMA((2,)),
            pltpu.SemaphoreType.DMA((kv_size,)),
            pltpu.SemaphoreType.DMA((kv_size,)),
        ],
        compiler_params=pltpu.CompilerParams(collective_id=0, has_side_effects=True),
        name="front",
    )(
        tokens,
        norm_gain.reshape(1, columns),
        *projections,
        beta_weight,
        decay_weight,
        decay_rate.reshape(1, heads_here),
    )


def back_kernel(
    kv_size,
    tp_size,
    model,
    mixed_heads,
    tokens,
    mlp_gain,
    out_weight,
    up_weight,
    down_weight,
    mixed_out,
    out_local,
    up_local,
    down_local,
    heads_all,
    first_parts,
    outgoing,
    incoming,
    hidden_mine,
    hidden_all,
    second_parts,
    part_send,
    local_sems,
    kv_sends,
    kv_receives,
    tp_sends,
    tp_receives,
):
    kv_index = lax.axis_index("kv")
    tp_index = lax.axis_index("tp")
    batch, columns = tokens.shape
    rows = batch // kv_size
    units = up_weight.shape[1]
    loads = []
    for place, (source, target) in enumerate(
        ((out_weight, out_local), (up_weight, up_local), (down_weight, down_local))
    ):
        load = pltpu.make_async_copy(source, target, local_sems.at[place])
        load.start()
        loads.append(load)
    greet(kv_size, tp_size)
    copies = send_all(
        "kv", kv_size, lambda peer: mixed_heads, heads_all, kv_sends.at[0], kv_receives.at[0]
    )
    heads_all[kv_index] = mixed_heads[...]
    loads[0].wait()
    for copy in copies:
        copy.wait()
    gathered = heads_all[...].astype(jnp.float32).reshape(batch, -1).astype(jnp.bfloat16)

    def exchange(partial, parts, turn):
        part_send[turn] = partial.astype(jnp.bfloat16)
        copies = send_all(
            "tp", tp_size, lambda peer: part_send.at[turn], parts,
            tp_sends.at[turn], tp_receives.at[turn],
        )
        parts[tp_index] = partial.astype(jnp.bfloat16)
        for copy in copies:
            copy.wait()
        return jnp.sum(parts[...].astype(jnp.float32), axis=0)

    attended = exchange(
        jnp.dot(gathered, out_local[...], preferred_element_type=jnp.float32), first_parts, 0
    )
    residual = (tokens[...].astype(jnp.float32) + attended).astype(jnp.bfloat16)
    resid_vals = residual.astype(jnp.float32)
    squares = jnp.sum(resid_vals * resid_vals, axis=1, keepdims=True)
    gain = mlp_gain[pl.ds(kv_index, 1), :]
    mlp_in = (resid_vals * gain).astype(jnp.bfloat16)
    loads[1].wait()
    pre_act = jnp.dot(mlp_in, up_local[...], preferred_element_type=jnp.float32)
    outgoing[:, :, 0:units] = pre_act.reshape(kv_size, rows, units).astype(jnp.bfloat16)
    outgoing[:, :, units:] = (
        jnp.broadcast_to(squares, (batch, LANES))
        .reshape(kv_size, rows, LANES)
        .astype(jnp.bfloat16)
    )
    copies = send_all(
        "kv", kv_size, lambda peer: outgoing.at[peer], incoming, kv_sends.at[1], kv_receives.at[1]
    )
    incoming[kv_index] = outgoing[kv_index]
    for copy in copies:
        copy.wait()
    total_squares = jnp.sum(incoming[:, :, units:].astype(jnp.float32), axis=0)[:, 0:1]
    summed = jnp.sum(incoming[:, :, 0:units].astype(jnp.float32), axis=0)
    active = jnp.maximum(summed * lax.rsqrt(total_squares / model + EPS), 0.0)
    hidden_mine[...] = (active * active).astype(jnp.bfloat16)
    copies = send_all(
        "kv", kv_size, lambda peer: hidden_mine, hidden_all, kv_sends.at[2], kv_receives.at[2]
    )
    hidden_all[kv_index] = hidden_mine[...]
    loads[2].wait()
    for copy in copies:
        copy.wait()
    hidden = hidden_all[...].astype(jnp.float32).reshape(batch, units).astype(jnp.bfloat16)
    mixed = exchange(
        jnp.dot(hidden, down_local[...], preferred_element_type=jnp.float32), second_parts, 1
    )
    mixed_out[...] = (resid_vals + mixed).astype(jnp.bfloat16)


def back(kv_size, tp_size, mixed_heads, tokens, mlp_gain, out_weight, up_weight, down_weight):
    batch, columns = tokens.shape
    rows, width = mixed_heads.shape
    units = up_weight.shape[1]
    half = jnp.bfloat16
    return pl.pallas_call(
        lambda *refs: back_kernel(kv_size, tp_size, columns * kv_size, *refs),
        out_shape=jax.ShapeDtypeStruct((batch, columns), half),
        in_specs=[VMEM_SPEC] * 3 + [ANY_SPEC] * 3,
        out_specs=VMEM_SPEC,
        scratch_shapes=[
            pltpu.VMEM((width, columns), half),
            pltpu.VMEM((columns, units), half),
            pltpu.VMEM((units, columns), half),
            pltpu.VMEM((kv_size, rows, width), half),
            pltpu.VMEM((tp_size, batch, columns), half),
            pltpu.VMEM((kv_size, rows, units + LANES), half),
            pltpu.VMEM((kv_size, rows, units + LANES), half),
            pltpu.VMEM((rows, units), half),
            pltpu.VMEM((kv_size, rows, units), half),
            pltpu.VMEM((tp_size, batch, columns), half),
            pltpu.VMEM((2, batch, columns), half),
            pltpu.SemaphoreType.DMA((3,)),
            pltpu.SemaphoreType.DMA((3, kv_size)),
            pltpu.SemaphoreType.DMA((3, kv_size)),
            pltpu.SemaphoreType.DMA((2, tp_size)),
            pltpu.SemaphoreType.DMA((2, tp_size)),
        ],
        compiler_params=pltpu.CompilerParams(collective_id=1, has_side_effects=True),
        name="back",
    )(
        mixed_heads,
        tokens,
        mlp_gain.reshape(kv_size, columns),
        out_weight,
        up_weight,
        down_weight,
    )


def body(
    kv_size,
    tp_size,
    tokens,
    norm_gain,
    query_weight,
    key_weight,
    value_weight,
    gate_weight,
    beta_weight,
    decay_weight,
    decay_rate,
    head_gain,
    carried_state,
    block_keys,
    block_values,
    block_beta,
    block_decay,
    live_count,
    out_weight,
    mlp_gain,
    up_weight,
    down_weight,
):
    seqs_here, heads_here, head_width = carried_state.shape[:3]
    queries, key_new, value_new, gate, beta_new, decay_new = front(
        kv_size,
        tokens,
        norm_gain,
        (query_weight, key_weight, value_weight, gate_weight),
        beta_weight,
        decay_weight,
        decay_rate,
    )
    per_head = (seqs_here, heads_here, head_width)
    readout, new_state = delta_block(
        queries.reshape(per_head),
        key_new.reshape(per_head),
        value_new.reshape(per_head),
        beta_new,
        decay_new,
        block_keys,
        block_values,
        block_beta,
        block_decay,
        live_count,
        carried_state,
    )
    scaled = (
        readout * lax.rsqrt(jnp.mean(readout * readout, axis=2, keepdims=True) + EPS) * head_gain
    )
    mixed_heads = (
        (scaled * gate.reshape(per_head))
        .reshape(seqs_here, heads_here * head_width)
        .astype(jnp.bfloat16)
    )
    mixed = back(
        kv_size, tp_size, mixed_heads, tokens, mlp_gain, out_weight, up_weight, down_weight
    )
    return (mixed, new_state)


def solution(mesh):
    placed = (
        P(None, "kv"),
        P("kv"),
        P("kv", "tp"),
        P("kv", "tp"),
        P("kv", "tp"),
        P("kv", "tp"),
        P(),
        P(),
        P("tp"),
        P(),
        P("kv", "tp", None, None),
        P("kv", "tp", None, None),
        P("kv", "tp", None, None),
        P("kv", "tp", None),
        P("kv", "tp", None),
        P("kv"),
        P("tp", "kv"),
        P(),
        P("kv", "tp"),
        P("tp", "kv"),
    )
    return jax.shard_map(
        functools.partial(body, mesh.shape["kv"], mesh.shape["tp"]),
        mesh=mesh,
        in_specs=placed,
        out_specs=(P(None, "kv"), P("kv", "tp", None, None)),
        check_vma=False,
    )
```
